32 devices in a mesh: ep: 16 (over z, y, x), tp: 2 (over core).
Axes of the slice: x: 2, y: 2, z: 4, core: 2. Of those that a mesh axis runs over, the one named last changes fastest.
Arguments:
- tokens: bfloat16 [512, 2048], P('ep'), may hold values from -6 to 6
- lengths: int32 [512], P('ep'), may hold values from 128 to 1024
- key_cache: bfloat16 [512, 1024, 256], P('ep', None, 'tp'), may hold values from -1000 to 1000
- value_cache: bfloat16 [512, 1024, 256], P('ep', None, 'tp'), may hold values from -6 to 6
- gate_cache: float32 [512, 16, 1024], P('ep', 'tp'), may hold values from -130 to 0, as said below
- mix_gain: float32 [2048], replicated, may hold values from 0.1 to 1.9
- query_weight: bfloat16 [2048, 1024], P(None, 'tp'), may hold values from -0.125 to 0.125
- key_weight: bfloat16 [2048, 256], P(None, 'tp'), may hold values from -0.125 to 0.125
- value_weight: bfloat16 [2048, 256], P(None, 'tp'), may hold values from -0.125 to 0.125
- forget_weight: bfloat16 [2048, 16], P(None, 'tp'), may hold values from -0.125 to 0.125
- out_weight: bfloat16 [1024, 2048], P('tp'), may hold values from -0.1875 to 0.1875
- expert_gain: float32 [2048], replicated, may hold values from 0.1 to 1.9
- routes: int32 [512, 2], P('ep'), may hold values from 0 to 7, all different within a row; in each aligned block of 32 rows (0 to 31, 32 to 63, ...) at most 12 rows name the same one
- route_weights: float32 [512, 2], P('ep'), may hold values from 0.2 to 1
- expert_gate: bfloat16 [2048, 65536], P(None, ('ep', 'tp')), may hold values from -0.125 to 0.125
- expert_up: bfloat16 [2048, 65536], P(None, ('ep', 'tp')), may hold values from -0.125 to 0.125
- expert_down: bfloat16 [65536, 2048], P(('ep', 'tp')), may hold values from -0.0625 to 0.0625
Outputs:
- layer_out: bfloat16 [512, 2048], P('ep')
The draws below stay inside these ranges and needn't reach their ends.
Inputs may be any that keep to these rules, and one draw needn't show every extreme that they name: `routes`: within the rows of one index of ep, no expert is named more than 12 times, and in every draw some expert is named exactly 12 times in some such rows; the 2 experts of a row differ. `gate_cache`: for each sequence and head the values never rise along the cache positions.
All inputs are finite; a program needn't handle non-finite values.
Results may differ from the reference program's by a relative error of at most 0.013.
Values may be sent and summed in bfloat16 or wider, within the bound.
A program may use at most 128 MiB of HBM per device.

```python
import math
import jax
import jax.numpy as jnp
import numpy as np
from jax import lax

D = 2048
HEADS = 16
KV_HEADS = 4
HD = 64
FF = 8192
EXPERTS = 8
TOP = 2
SEQ_DEV = 32
CACHE_POSITIONS = 1024
CAP = 12
SEQUENCE_TOTAL = 512
N_EP = 16
N_TP = 2


def draw_gate_cache(key, part):
    key_fragments = jax.random.split(jax.random.fold_in(key, 11), 7)
    order = jax.random.permutation(key_fragments[0], HEADS)
    slow = order < HEADS // 2
    slow_rate = jax.random.uniform(key_fragments[1], (SEQUENCE_TOTAL, HEADS), jnp.float32, 0.1, 0.5) / CACHE_POSITIONS
    fast_rate = jnp.exp(jax.random.uniform(key_fragments[2], (SEQUENCE_TOTAL, HEADS), jnp.float32, jnp.log(1.0 / 100.0), jnp.log(1.0 / 30.0)))
    rate = jnp.where(slow[None, :], slow_rate, fast_rate)
    seq_factor = jnp.exp(jax.random.uniform(key_fragments[3], (SEQUENCE_TOTAL, 1, 1), jnp.float32, -0.7, 0.7))
    rough = jax.random.uniform(key_fragments[4], (SEQUENCE_TOTAL, HEADS, CACHE_POSITIONS), jnp.float32, 0.4, 1.6)
    step_log_gates = -rate[:, :, None] * seq_factor * rough
    spike_position = jax.random.randint(key_fragments[5], (SEQUENCE_TOTAL, 3), 0, CACHE_POSITIONS)
    decay_amounts = jax.random.uniform(key_fragments[6], (SEQUENCE_TOTAL, 3), jnp.float32, 0.2, 0.4)
    cache_locations = jnp.arange(CACHE_POSITIONS, dtype=jnp.int32)
    spike_events = jnp.sum(jnp.where(cache_locations[None, None, :] == spike_position[:, :, None], jnp.log(1.0 - decay_amounts)[:, :, None], 0.0), axis=1)
    step_log_gates = step_log_gates + spike_events[:, None, :]
    return jnp.cumsum(step_log_gates, axis=-1).astype(jnp.float32)


def draw_key_cache(key, part):
    key_fragments = jax.random.split(jax.random.fold_in(key, 23), 1)
    base = jnp.clip(jax.random.normal(key_fragments[0], (SEQUENCE_TOTAL, CACHE_POSITIONS, KV_HEADS * HD), jnp.float32), -6.0, 6.0)
    return base.astype(jnp.bfloat16)


def with_ends(values, rng, smallest, largest):
    shape = values.shape
    place = [jax.random.randint(jax.random.fold_in(rng, axis), (), 0, shape[axis]) for axis in range(len(shape))]
    values = values.at[tuple(place)].set(smallest)
    longest = shape.index(max(shape))
    place[longest] = (place[longest] + 1) % shape[longest]
    return values.at[tuple(place)].set(largest)


def levels(rng, dims, cuts, smallest, top_value):
    level = 1.0
    for axis_at, shards_of in cuts:
        steps = jax.random.uniform(jax.random.fold_in(jax.random.fold_in(rng, 6), axis_at), (shards_of,), jnp.float32, smallest / len(cuts), top_value / len(cuts))
        level = level * jnp.repeat(jnp.exp(steps), dims[axis_at] // shards_of).reshape((-1,) + (1,) * (len(dims) - 1 - axis_at))
    return level


def deal_out(key, own, number, rows, count, top, bound, lean):
    sequence = jax.random.permutation(key, count)
    crowded, usual = shares(count, rows * top, bound, lean, True), shares(count, rows * top, bound, lean, False)
    places = jnp.arange(count)

    def named(sizes, rotation):
        used = int((sizes > 0).sum())
        fixed = max(1, used // 4)
        shifted = fixed + (places - fixed + rotation * (used - fixed)) % max(1, count - fixed)
        return jnp.zeros((count,), jnp.int32).at[sequence[jnp.where(places < fixed, places, shifted)]].set(jnp.asarray(sizes, jnp.int32))

    sizes = jnp.where(number % 4 == 0, named(crowded, number // 4), named(usual, number - number // 4 - 1))
    mixed = jax.random.permutation(jax.random.fold_in(own, 3), count)
    source_of, taker = mixed[0:count // 2 * 2:2], mixed[1:count // 2 * 2:2]
    room = jnp.minimum(sizes[source_of] - 1, bound - sizes[taker]) // 2
    room = jnp.where((source_of == sequence[0]) | (taker == sequence[0]) | (sizes[taker] == 0), 0, jnp.maximum(room, 0))
    shifted = jax.random.randint(jax.random.fold_in(own, 4), (count // 2,), 0, 1 << 20) % (room + 1)
    sizes = sizes.at[source_of].add(-shifted).at[taker].add(shifted)
    members = jnp.searchsorted(jnp.cumsum(sizes), jnp.arange(rows * top), side="right").astype(jnp.int32)
    listing = members.reshape(top, rows).T
    listing = listing[jax.random.permutation(jax.random.fold_in(own, 1), rows)]
    rotation = jax.random.randint(jax.random.fold_in(own, 2), (rows, 1), 0, top)
    return jnp.take_along_axis(listing, (jnp.arange(top)[None, :] + rotation) % top, axis=1)


def shares(count, total, reach, lean, full):
    loads = [(1 << 20) // math.isqrt(grade ** lean) + 1 for grade in range(1, count + 1)]
    largest = reach if full else min(reach, max(-(-total // count), total * loads[0] // sum(loads)))
    least = 1 if total - largest >= count - 1 else 0
    counts, rest = [largest] + [least] * (count - 1), total - largest - least * (count - 1)
    while rest > 0:
        candidates = [i for i in range(1, count) if counts[i] < largest] or [i for i in range(1, count) if counts[i] < reach]
        pool, budget = sum([loads[i] for i in candidates]), rest
        for i in candidates:
            addition = min(reach - counts[i], max(1, budget * loads[i] // pool), rest)
            counts[i] = counts[i] + addition
            rest = rest - addition
    return np.array(counts)


def scatter_about(own_key, extent, scale, reach, cuts=(), held_as=jnp.bfloat16):
    array = jax.random.normal(own_key, extent, jnp.float32) * scale
    if len(cuts) > 0:
        array = levels(own_key, extent, cuts, -0.22, 0.18) * array
    return jnp.clip(array, min=-reach, max=reach).astype(held_as)


def setup_inputs(seed: int = 0) -> dict:
    splits = jax.random.split(jax.random.key(seed), 18)
    tokens = scatter_about(splits[0], (SEQUENCE_TOTAL, D), 1.0, 6.0, ((0, 16),))
    lengths = with_ends(jax.random.randint(splits[1], (SEQUENCE_TOTAL,), CACHE_POSITIONS // 8, CACHE_POSITIONS + 1), jax.random.fold_in(splits[1], 1), CACHE_POSITIONS // 8, CACHE_POSITIONS).astype(jnp.int32)
    key_cache = draw_key_cache(jax.random.fold_in(splits[17], 71), 0)
    value_cache = scatter_about(splits[3], (SEQUENCE_TOTAL, CACHE_POSITIONS, KV_HEADS * HD), 1.0, 6.0, ((0, 16), (2, 2)))
    gate_cache = draw_gate_cache(jax.random.fold_in(splits[17], 71), 0)
    mix_gain = jnp.clip(1.0 + 0.18 * jax.random.normal(splits[5], (D,), jnp.float32), 0.1, 1.9)
    query_weight = scatter_about(splits[6], (D, HEADS * HD), D ** -0.5, 0.125, ((1, 2),))
    key_weight = scatter_about(splits[7], (D, KV_HEADS * HD), D ** -0.5, 0.125, ((1, 2),))
    value_weight = scatter_about(splits[8], (D, KV_HEADS * HD), D ** -0.5, 0.125, ((1, 2),))
    forget_weight = scatter_about(splits[9], (D, HEADS), D ** -0.5, 0.125, ((1, 2),))
    out_weight = scatter_about(splits[10], (HEADS * HD, D), (HEADS * HD) ** -0.5, 0.1875, ((0, 2),))
    expert_gain = jnp.clip(1.0 + 0.18 * jax.random.normal(splits[11], (D,), jnp.float32), 0.1, 1.9)
    routes_keys = jax.random.split(jax.random.fold_in(splits[12], 1), SEQUENCE_TOTAL // SEQ_DEV)
    routes_turns = jax.random.permutation(jax.random.fold_in(splits[12], 3), SEQUENCE_TOTAL // SEQ_DEV)
    routes = jax.vmap(lambda own, number: deal_out(jax.random.fold_in(splits[12], 2), own, number, SEQ_DEV, EXPERTS, TOP, CAP, 2))(routes_keys, routes_turns).reshape((SEQUENCE_TOTAL, TOP))
    route_weights = jnp.clip(0.2 + 0.8 * jax.random.uniform(splits[13], (SEQUENCE_TOTAL, TOP), jnp.float32) ** levels(splits[13], (SEQUENCE_TOTAL, TOP), ((0, 16),), -0.2, 0.2), 0.2, 1.0)
    expert_gate = scatter_about(splits[14], (D, EXPERTS * FF), D ** -0.5, 0.125, ((1, 32),))
    expert_up = scatter_about(splits[15], (D, EXPERTS * FF), D ** -0.5, 0.125, ((1, 32),))
    expert_down = scatter_about(splits[16], (EXPERTS * FF, D), FF ** -0.5, 0.0625, ((0, 32),))
    return dict(tokens=tokens, lengths=lengths, key_cache=key_cache, value_cache=value_cache, gate_cache=gate_cache, mix_gain=mix_gain, query_weight=query_weight, key_weight=key_weight, value_weight=value_weight, forget_weight=forget_weight, out_weight=out_weight, expert_gain=expert_gain, routes=routes, route_weights=route_weights, expert_gate=expert_gate, expert_up=expert_up, expert_down=expert_down)


eps = 1e-06

def normed(values, gain):
    floats = values.astype(jnp.float32)
    return floats * lax.rsqrt(lax.optimization_barrier(jnp.mean(floats * floats, axis=-1, keepdims=True)) + eps) * gain

def attend(pack):
    queries, key_new, value_new, log_gate, key_rows, value_rows, cumulative, length = pack
    seq_count, head_count, head_size = queries.shape
    kv_count = key_new.shape[1]
    group_size = head_count // kv_count
    cache_locations = key_rows.shape[1]
    factor = head_size ** (-0.5)
    grouped = queries.reshape(seq_count, kv_count, group_size, head_size).astype(jnp.float32)
    key_split = key_rows.reshape(seq_count, cache_locations, kv_count, head_size).astype(jnp.float32)
    value_split = value_rows.reshape(seq_count, cache_locations, kv_count, head_size).astype(jnp.float32)
    scores = jnp.einsum('skgd,spkd->skgp', grouped, key_split).reshape(seq_count, head_count, cache_locations) * factor
    positions = jnp.arange(cache_locations, dtype=jnp.int32)
    latest = lax.optimization_barrier(jnp.sum(jnp.where(positions[None, None, :] == (length - 1)[:, None, None], cumulative, 0.0), axis=-1))
    scores = scores + (latest + log_gate)[..., None] - cumulative
    valid = positions[None, None, :] < length[:, None, None]
    scores = jnp.where(valid, scores, -jnp.inf)
    own_score = jnp.einsum('skgd,skd->skg', grouped, key_new.astype(jnp.float32)).reshape(seq_count, head_count) * factor
    highest = jnp.maximum(lax.optimization_barrier(jnp.max(scores, axis=-1)), own_score)
    raised = jnp.exp(scores - highest[..., None])
    own_raised = jnp.exp(own_score - highest)
    denominator = lax.optimization_barrier(jnp.sum(raised, axis=-1)) + own_raised
    weights = (raised / denominator[..., None]).astype(jnp.bfloat16)
    own_weight = (own_raised / denominator).astype(jnp.bfloat16)
    mixed = jnp.einsum('skgp,spkd->skgd', weights.reshape(seq_count, kv_count, group_size, cache_locations).astype(jnp.float32), value_split)
    mixed = mixed + own_weight.reshape(seq_count, kv_count, group_size)[..., None].astype(jnp.float32) * value_new.astype(jnp.float32)[:, :, None, :]
    return mixed.reshape(seq_count, head_count * head_size).astype(jnp.bfloat16)

def reference(tokens, lengths, key_cache, value_cache, gate_cache, mix_gain, query_weight, key_weight, value_weight, forget_weight, out_weight, expert_gain, routes, route_weights, expert_gate, expert_up, expert_down):
    normal_in = normed(tokens, mix_gain).astype(jnp.bfloat16)
    queries = jnp.dot(normal_in, query_weight, preferred_element_type=jnp.float32).astype(jnp.bfloat16).reshape(N_EP, SEQ_DEV, HEADS, HD)
    key_new = jnp.dot(normal_in, key_weight, preferred_element_type=jnp.float32).astype(jnp.bfloat16).reshape(N_EP, SEQ_DEV, KV_HEADS, HD)
    value_new = jnp.dot(normal_in, value_weight, preferred_element_type=jnp.float32).astype(jnp.bfloat16).reshape(N_EP, SEQ_DEV, KV_HEADS, HD)
    log_gate = jax.nn.log_sigmoid(jnp.dot(normal_in, forget_weight, preferred_element_type=jnp.float32)).reshape(N_EP, SEQ_DEV, HEADS)
    mixed = lax.map(attend, (queries, key_new, value_new, log_gate, key_cache.reshape(N_EP, SEQ_DEV, CACHE_POSITIONS, KV_HEADS * HD), value_cache.reshape(N_EP, SEQ_DEV, CACHE_POSITIONS, KV_HEADS * HD), gate_cache.reshape(N_EP, SEQ_DEV, HEADS, CACHE_POSITIONS), lengths.reshape(N_EP, SEQ_DEV)))
    mixed = mixed.reshape(SEQUENCE_TOTAL, HEADS * HD)
    split = HEADS * HD // N_TP
    summed = tokens.astype(jnp.float32)
    for group_index in range(N_TP):
        product = jnp.dot(mixed[:, group_index * split:(group_index + 1) * split], out_weight[group_index * split:(group_index + 1) * split], preferred_element_type=jnp.float32)
        summed = summed + lax.optimization_barrier(product.astype(jnp.bfloat16)).astype(jnp.float32)
    residual = summed.astype(jnp.bfloat16)
    expert_in = normed(residual, expert_gain).astype(jnp.bfloat16)
    flat_routes = routes.reshape(N_EP, SEQ_DEV * TOP)
    one_hot = (flat_routes[..., None] == jnp.arange(EXPERTS, dtype=jnp.int32)).astype(jnp.int32)
    slot_index = lax.optimization_barrier(jnp.sum((jnp.cumsum(one_hot, axis=1) - 1) * one_hot, axis=-1))
    repeated = jnp.repeat(expert_in.reshape(N_EP, SEQ_DEV, D), TOP, axis=1).astype(jnp.float32)
    pieces = N_EP // EXPERTS
    quarter = FF // (pieces * N_TP)

    def one_expert(expert):
        chosen = (flat_routes == expert)[:, None, :] & (slot_index[:, None, :] == jnp.arange(CAP, dtype=jnp.int32)[None, :, None])
        rows_in = jnp.einsum('ncr,nrd->ncd', chosen.astype(jnp.float32), repeated).astype(jnp.bfloat16).reshape(N_EP * CAP, D)
        w_gate = lax.dynamic_slice_in_dim(expert_gate, expert * FF, FF, 1)
        w_up = lax.dynamic_slice_in_dim(expert_up, expert * FF, FF, 1)
        w_down = lax.dynamic_slice_in_dim(expert_down, expert * FF, FF, 0)
        gate_out = jnp.dot(rows_in, w_gate, preferred_element_type=jnp.float32)
        up_out = jnp.dot(rows_in, w_up, preferred_element_type=jnp.float32)
        hidden = (jax.nn.silu(gate_out) * up_out).astype(jnp.bfloat16)
        halves = jnp.einsum('rbtf,btfd->rbtd', hidden.reshape(N_EP * CAP, pieces, N_TP, quarter).astype(jnp.float32), w_down.reshape(pieces, N_TP, quarter, D).astype(jnp.float32))
        halves = lax.optimization_barrier(halves.astype(jnp.bfloat16)).astype(jnp.float32)
        blocks = lax.optimization_barrier(lax.optimization_barrier(jnp.sum(halves, axis=2)).astype(jnp.bfloat16)).astype(jnp.float32)
        return lax.optimization_barrier(jnp.sum(blocks, axis=1))
    results = lax.map(one_expert, jnp.arange(EXPERTS, dtype=jnp.int32))
    row_index = flat_routes * (N_EP * CAP) + jnp.arange(N_EP, dtype=jnp.int32)[:, None] * CAP + slot_index
    picked = jnp.take(results.reshape(EXPERTS * N_EP * CAP, D), row_index.reshape(-1).astype(jnp.int32), axis=0).reshape(SEQUENCE_TOTAL, TOP, D)
    mixture = lax.optimization_barrier(jnp.sum(picked * route_weights[..., None], axis=1))
    return (residual.astype(jnp.float32) + mixture).astype(jnp.bfloat16)
```

```python
import functools

import jax
import jax.numpy as jnp
from jax import lax
from jax.experimental import pallas as pl
from jax.experimental.pallas import tpu as pltpu
from jax.sharding import PartitionSpec as P

HD = 64
EXPERTS = 8
CAP = 12
QUARTERS = 4
GROUP = 4
STEP_SEQS = 4
MESH = pl.DeviceIdType.MESH
F32 = jnp.float32
BF16 = jnp.bfloat16

eps = 1e-06


def normed(values, gain):
    floats = values.astype(F32)
    return floats * lax.rsqrt(jnp.mean(floats * floats, axis=-1, keepdims=True) + eps) * gain


def attention_kernel(
    len_ref, tok_ref, gain_ref, wq_ref, wk_ref, wv_ref, wf_ref, wo_ref, k_ref, v_ref, g_ref,
    out_ref, q_sc, lg_sc, kn_sc, vn_sc, mix_sc,
):
    step = pl.program_id(0)
    seqs = tok_ref.shape[0]
    heads = g_ref.shape[1]
    lanes = k_ref.shape[2]
    positions = k_ref.shape[1]
    group = heads // (lanes // HD)
    per_slice = lanes // HD
    lane = lax.broadcasted_iota(jnp.int32, (seqs, lanes), 1)

    @pl.when(step == 0)
    def _():
        x = normed(tok_ref[...], gain_ref[...]).astype(BF16)
        q = jnp.dot(x, wq_ref[...], preferred_element_type=F32).astype(BF16).astype(F32)
        kn_sc[...] = jnp.dot(x, wk_ref[...], preferred_element_type=F32).astype(BF16).astype(F32)
        vn_sc[...] = jnp.dot(x, wv_ref[...], preferred_element_type=F32).astype(BF16).astype(F32)
        gates = jnp.dot(x, wf_ref[...], preferred_element_type=F32)
        gates = jnp.minimum(gates, 0.0) - jnp.log1p(jnp.exp(-jnp.abs(gates)))
        for h in range(heads):
            base = (h // per_slice) * lanes
            part = q[:, base:base + lanes]
            at, want = h % per_slice, h // group
            if at != want:
                part = pltpu.roll(part, (want - at) * HD % lanes, 1)
            part = jnp.where(lane // HD == want, part, 0.0)
            q_sc[:, h, :] = part
            lg_sc[:, h, :] = jnp.broadcast_to(gates[:, h:h + 1], (seqs, lanes))

    pos = lax.broadcasted_iota(jnp.int32, (heads, positions), 1)
    factor = HD ** (-0.5)
    for j in range(k_ref.shape[0]):
        s = step * k_ref.shape[0] + j
        length = len_ref[s]
        q = q_sc[s]
        g = g_ref[j]
        scores = lax.dot_general(
            q.astype(BF16), k_ref[j], (((1,), (1,)), ((), ())), preferred_element_type=F32
        ) * factor
        latest = jnp.sum(jnp.where(pos == length - 1, g, 0.0), axis=-1, keepdims=True)
        scores = scores + (latest + lg_sc[s][:, 0:1]) - g
        scores = jnp.where(pos < length, scores, -jnp.inf)
        own = jnp.sum(q * kn_sc[pl.ds(s, 1), :], axis=-1, keepdims=True) * factor
        top = jnp.maximum(jnp.max(scores, axis=-1, keepdims=True), own)
        raised = jnp.exp(scores - top)
        own_raised = jnp.exp(own - top)
        inverse = 1.0 / (jnp.sum(raised, axis=-1, keepdims=True) + own_raised)
        weights = (raised * inverse).astype(BF16)
        own_weight = (own_raised * inverse).astype(BF16).astype(F32)
        mix_sc[s] = (
            jnp.dot(weights, v_ref[j], preferred_element_type=F32)
            + own_weight * vn_sc[pl.ds(s, 1), :]
        )

    @pl.when(step == pl.num_programs(0) - 1)
    def _():
        pieces = []
        for base in range(0, heads, per_slice):
            joined = None
            for h in range(base, base + per_slice):
                part = mix_sc[:, h, :]
                at, want = h // group, h % per_slice
                if at != want:
                    part = pltpu.roll(part, (want - at) * HD % lanes, 1)
                joined = part if joined is None else jnp.where(lane // HD == want, part, joined)
            pieces.append(joined.astype(BF16))
        mixed = jnp.concatenate(pieces, axis=1)
        out_ref[...] = jnp.dot(mixed, wo_ref[...], preferred_element_type=F32).astype(BF16)


def attention(tokens, lengths, key_cache, value_cache, gate_cache, mix_gain, wq, wk, wv, wf, wo):
    seqs, width = tokens.shape
    _, positions, lanes = key_cache.shape
    heads = gate_cache.shape[1]
    whole = lambda a: pl.BlockSpec(a.shape, lambda i: (0,) * a.ndim)
    gain = mix_gain.reshape(1, width)
    return pl.pallas_call(
        attention_kernel,
        grid=(seqs // STEP_SEQS,),
        out_shape=jax.ShapeDtypeStruct((seqs, width), BF16),
        in_specs=[pl.BlockSpec(memory_space=pltpu.SMEM)]
        + [whole(a) for a in (tokens, gain, wq, wk, wv, wf, wo)]
        + [
            pl.BlockSpec((STEP_SEQS, positions, lanes), lambda i: (i, 0, 0)),
            pl.BlockSpec((STEP_SEQS, positions, lanes), lambda i: (i, 0, 0)),
            pl.BlockSpec((STEP_SEQS, heads, positions), lambda i: (i, 0, 0)),
        ],
        out_specs=pl.BlockSpec((seqs, width), lambda i: (0, 0)),
        scratch_shapes=[
            pltpu.VMEM((seqs, heads, lanes), F32),
            pltpu.VMEM((seqs, heads, lanes), F32),
            pltpu.VMEM((seqs, lanes), F32),
            pltpu.VMEM((seqs, lanes), F32),
            pltpu.VMEM((seqs, heads, lanes), F32),
        ],
        compiler_params=pltpu.CompilerParams(
            dimension_semantics=("arbitrary",), vmem_limit_bytes=48 * 1024 * 1024
        ),
        name="attention",
    )(lengths, tokens, gain, wq, wk, wv, wf, wo, key_cache, value_cache, gate_cache)


def moe_kernel(
    n_ep, part_ref, tok_ref, gain_ref, routes_ref, rw_ref, wg_hbm, wu_hbm, wd_hbm, out_ref,
    wg, wu, wd, peer_part, residual, normal, outgoing, rows, x_sc, h_sc, stage, s_other, s_own,
    t_in, blocks, u_in, finals, returned,
    w_sem, part_sem, col_send, fan_send, mate_send, row_recv, t_send, t_recv, u_send, u_recv,
    ret_send, ret_recv, out_sem,
):
    me = lax.axis_index("ep")
    t = lax.axis_index("tp")
    pieces = n_ep // EXPERTS
    e, p = me // pieces, lax.rem(me, pieces)
    mate = (me, 1 - t)
    order = (4, 3, 5, 2, 6, 1, 7)
    seqs, width = tok_ref.shape
    half = width // 2
    quarter = half // QUARTERS
    ff = wg_hbm.shape[1]

    def column(k):
        return lax.rem(e + k, EXPERTS)

    def peer(i):
        return lax.rem(p + i, pieces)

    weight_copies = [
        pltpu.make_async_copy(src, dst, w_sem.at[i])
        for i, (src, dst) in enumerate(((wg_hbm, wg), (wu_hbm, wu), (wd_hbm, wd)))
    ]
    for copy in weight_copies:
        copy.start()

    barrier = pltpu.get_barrier_semaphore()
    pl.semaphore_signal(barrier, inc=1, device_id=mate, device_id_type=MESH)
    for i in range(1, pieces):
        pl.semaphore_signal(barrier, inc=1, device_id=(e * pieces + peer(i), t), device_id_type=MESH)
    for k in range(1, EXPERTS):
        pl.semaphore_signal(barrier, inc=1, device_id=(column(k) * pieces + p, t), device_id_type=MESH)
    pl.semaphore_wait(barrier, 1 + (pieces - 1) + (EXPERTS - 1))

    def send(src, dst, send_sem, recv_sem, device):
        copy = pltpu.make_async_remote_copy(
            src_ref=src, dst_ref=dst, send_sem=send_sem, recv_sem=recv_sem,
            device_id=device, device_id_type=MESH,
        )
        copy.start()
        return copy

    def arrived(dst, send_sem, recv_sem):
        pltpu.make_async_remote_copy(
            src_ref=dst, dst_ref=dst, send_sem=send_sem, recv_sem=recv_sem,
            device_id=mate, device_id_type=MESH,
        ).wait_recv()

    sent = [send(part_ref, peer_part, part_sem.at[0], part_sem.at[1], mate)]

    block = QUARTERS * CAP
    columns = EXPERTS * block
    col = lax.broadcasted_iota(jnp.int32, (seqs, columns), 1)
    col_expert = col // block
    col_slot = lax.rem(col, CAP)
    r0, r1 = routes_ref[:, 0:1], routes_ref[:, 1:2]
    first, second = r0 == col_expert, r1 == col_expert
    named = jnp.where(first | second, 1.0, 0.0)
    before = jnp.where(
        lax.broadcasted_iota(jnp.int32, (seqs, seqs), 1)
        < lax.broadcasted_iota(jnp.int32, (seqs, seqs), 0), 1.0, 0.0,
    )
    slot = jnp.dot(before.astype(BF16), named.astype(BF16), preferred_element_type=F32)
    chosen = jnp.where(slot == col_slot.astype(F32), named, 0.0)
    weight = jnp.where(first, rw_ref[:, 0:1], jnp.where(second, rw_ref[:, 1:2], 0.0)) * chosen
    col_quarter = lax.rem(col, block) // CAP
    spread = lambda a: jnp.concatenate(
        [jnp.where(col_quarter == q, a, 0.0) for q in range(QUARTERS)], axis=0
    )
    dispatch = spread(chosen).astype(BF16)
    weight = spread(weight)
    weight_high = weight.astype(BF16)
    weight_low = (weight - weight_high.astype(F32)).astype(BF16)

    size = GROUP * block
    out_row = lax.broadcasted_iota(jnp.int32, (size, size), 0)
    in_row = lax.broadcasted_iota(jnp.int32, (size, size), 1)

    def unpacked(r):
        q = r // (GROUP * CAP)
        i = lax.rem(r, GROUP * CAP) // CAP
        return i * block + q * CAP + lax.rem(r, CAP)

    unpack = jnp.where(in_row == unpacked(out_row), 1.0, 0.0).astype(BF16)
    pack = jnp.where(out_row == unpacked(in_row), 1.0, 0.0).astype(BF16)

    arrived(peer_part, part_sem.at[0], part_sem.at[1])
    total = tok_ref[...].astype(F32) + (part_ref[...].astype(F32) + peer_part[...].astype(F32))
    rounded = total.astype(BF16)
    residual[...] = rounded
    normal[...] = normed(rounded, gain_ref[...]).astype(BF16)

    start = pl.multiple_of(t * half, half)
    mine = normal[:, pl.ds(start, half)]
    stacked = jnp.concatenate(
        [mine[:, q * quarter:(q + 1) * quarter] for q in range(QUARTERS)], axis=0
    )
    outgoing[...] = lax.dot_general(
        dispatch, stacked, (((0,), (0,)), ((), ())), preferred_element_type=F32
    ).astype(BF16).reshape(EXPERTS, block, quarter)

    own_row = p * EXPERTS + e
    for n, k in enumerate(order):
        a = column(k)
        sent.append(send(outgoing.at[a], rows.at[own_row, t], col_send.at[n],
                         row_recv.at[own_row, t], (a * pieces + p, t)))
    fans = 0
    mates = 0

    def fan(src, r):
        nonlocal fans
        for i in range(1, pieces):
            sent.append(send(src, rows.at[r, t], fan_send.at[fans], row_recv.at[r, t],
                             (e * pieces + peer(i), t)))
            fans += 1

    def to_mate(src, r):
        nonlocal mates
        sent.append(send(src, rows.at[r, t], mate_send.at[mates], row_recv.at[r, t], mate))
        mates += 1

    fan(outgoing.at[e], own_row)
    to_mate(outgoing.at[e], own_row)
    rows[own_row, t] = outgoing[e]
    inbound = [lax.rem(e + EXPERTS - k, EXPERTS) for k in order]
    for n, a in enumerate(inbound):
        r = p * EXPERTS + a
        arrived(rows.at[r, t], col_send.at[0], row_recv.at[r, t])
        fan(rows.at[r, t], r)
        to_mate(rows.at[r, t], r)
    for a in [e] + inbound:
        for i in range(1, pieces):
            r = peer(i) * EXPERTS + a
            arrived(rows.at[r, t], col_send.at[0], row_recv.at[r, t])
            to_mate(rows.at[r, t], r)
    for i in range(pieces):
        for a in [e] + inbound:
            r = peer(i) * EXPERTS + a
            arrived(rows.at[r, 1 - t], col_send.at[0], row_recv.at[r, 1 - t])

    groups = n_ep // GROUP
    group_rows = GROUP * CAP
    for g in range(groups):
        for h in range(2):
            packed = rows[g * GROUP:(g + 1) * GROUP, h].reshape(size, quarter)
            moved = jnp.dot(unpack, packed, preferred_element_type=F32).astype(BF16)
            for q in range(QUARTERS):
                x_sc[g * group_rows:(g + 1) * group_rows,
                     h * half + q * quarter:h * half + (q + 1) * quarter] = (
                    moved[q * group_rows:(q + 1) * group_rows])

    weight_copies[0].wait()
    weight_copies[1].wait()
    chunk = 256

    @pl.loop(0, ff // chunk)
    def _(c):
        at = pl.ds(pl.multiple_of(c * chunk, chunk), chunk)
        x = x_sc[...]
        gate = jnp.dot(x, wg[:, at], preferred_element_type=F32)
        up = jnp.dot(x, wu[:, at], preferred_element_type=F32)
        h_sc[:, at] = (gate * (1.0 / (1.0 + jnp.exp(-gate))) * up).astype(BF16)

    weight_copies[2].wait()

    def down(h, into):
        for q in range(QUARTERS):
            at = pl.ds(pl.multiple_of(h * half + q * quarter, quarter), quarter)
            y = jnp.dot(h_sc[...], wd[:, at], preferred_element_type=F32).astype(BF16)
            for g in range(groups):
                stage[g, q * group_rows:(q + 1) * group_rows] = (
                    y[g * group_rows:(g + 1) * group_rows])
        for g in range(groups):
            into[g * GROUP:(g + 1) * GROUP] = jnp.dot(
                pack, stage[g], preferred_element_type=F32
            ).astype(BF16).reshape(GROUP, block, quarter)

    down(1 - t, s_other)
    turns = list(range(1, pieces)) + [0]
    for i in turns:
        at = pl.ds(peer(i) * EXPERTS, EXPERTS)
        sent.append(send(s_other.at[at], t_in.at[at], t_send.at[i], t_recv.at[i], mate))
    down(t, s_own)
    backward = [column(k) for k in order] + [e]
    for i in turns:
        at = pl.ds(peer(i) * EXPERTS, EXPERTS)
        arrived(t_in.at[at], t_send.at[0], t_recv.at[i])
        for n, a in enumerate(backward):
            r = peer(i) * EXPERTS + a
            blocks[r] = (s_own[r].astype(F32) + t_in[r].astype(F32)).astype(BF16)
            if i > 0:
                sent.append(send(blocks.at[r], u_in.at[i - 1, a], u_send.at[i - 1, n],
                                 u_recv.at[i - 1, a], (e * pieces + peer(i), t)))
    for n, a in enumerate(backward):
        summed = blocks[p * EXPERTS + a].astype(F32)
        for i in range(1, pieces):
            arrived(u_in.at[i - 1, a], u_send.at[0, 0], u_recv.at[i - 1, a])
            summed = summed + u_in[i - 1, a].astype(F32)
        finals[a] = summed.astype(BF16)
        if n < len(order):
            sent.append(send(finals.at[a], returned.at[e], ret_send.at[n], ret_recv.at[e],
                             (a * pieces + p, t)))
    returned[e] = finals[e]
    for a in inbound:
        arrived(returned.at[a], ret_send.at[0], ret_recv.at[a])
    back = returned[...].reshape(columns, quarter)
    mixture = (
        jnp.dot(weight_high, back, preferred_element_type=F32)
        + jnp.dot(weight_low, back, preferred_element_type=F32)
    )
    for q in range(QUARTERS):
        at = pl.ds(pl.multiple_of(start + q * quarter, quarter), quarter)
        out_ref[:, at] = (
            residual[:, at].astype(F32) + mixture[q * seqs:(q + 1) * seqs]
        ).astype(BF16)
    here = pl.ds(start, half)
    there = pl.ds(pl.multiple_of((1 - t) * half, half), half)
    sent.append(send(out_ref.at[:, here], out_ref.at[:, here], out_sem.at[0], out_sem.at[1], mate))
    arrived(out_ref.at[:, there], out_sem.at[0], out_sem.at[1])
    for copy in sent:
        copy.wait_send()


def moe(n_ep, partial, tokens, expert_gain, routes, route_weights, gate, up, down):
    seqs, width = tokens.shape
    pieces = n_ep // EXPERTS
    half = width // 2
    quarter = half // QUARTERS
    block = QUARTERS * CAP
    ff = gate.shape[1]
    count = n_ep * CAP
    vmem = pl.BlockSpec(memory_space=pltpu.VMEM)
    hbm = pl.BlockSpec(memory_space=pl.ANY)
    dma = lambda *s: pltpu.SemaphoreType.DMA(s)
    buf = lambda *s: pltpu.VMEM(s, BF16)
    return pl.pallas_call(
        functools.partial(moe_kernel, n_ep),
        out_shape=jax.ShapeDtypeStruct((seqs, width), BF16),
        in_specs=[vmem] * 5 + [hbm] * 3,
        out_specs=vmem,
        scratch_shapes=[
            buf(*gate.shape), buf(*up.shape), buf(*down.shape),
            buf(seqs, width), buf(seqs, width), buf(seqs, width),
            buf(EXPERTS, block, quarter),
            buf(n_ep, 2, block, quarter),
            buf(count, width), buf(count, ff),
            buf(n_ep // GROUP, GROUP * block, quarter),
            buf(n_ep, block, quarter), buf(n_ep, block, quarter),
            buf(n_ep, block, quarter), buf(n_ep, block, quarter),
            buf(max(1, pieces - 1), EXPERTS, block, quarter),
            buf(EXPERTS, block, quarter), buf(EXPERTS, block, quarter),
            dma(3), dma(2), dma(EXPERTS), dma(max(1, EXPERTS * (pieces - 1))), dma(n_ep),
            dma(n_ep, 2), dma(pieces), dma(pieces),
            dma(max(1, pieces - 1), EXPERTS), dma(max(1, pieces - 1), EXPERTS),
            dma(EXPERTS), dma(EXPERTS), dma(2),
        ],
        compiler_params=pltpu.CompilerParams(
            collective_id=0, has_side_effects=True, vmem_limit_bytes=60 * 1024 * 1024
        ),
        name="experts",
    )(partial, tokens, expert_gain.reshape(1, width), routes, route_weights, gate, up, down)


def on_device(
    n_ep, tokens, lengths, key_cache, value_cache, gate_cache, mix_gain, query_weight, key_weight,
    value_weight, forget_weight, out_weight, expert_gain, routes, route_weights, expert_gate,
    expert_up, expert_down,
):
    partial = attention(
        tokens, lengths, key_cache, value_cache, gate_cache, mix_gain, query_weight, key_weight,
        value_weight, forget_weight, out_weight,
    )
    return moe(n_ep, partial, tokens, expert_gain, routes, route_weights,
               expert_gate, expert_up, expert_down)


def solution(mesh):
    return jax.shard_map(
        functools.partial(on_device, mesh.shape["ep"]),
        mesh=mesh,
        in_specs=(
            P("ep", None),
            P("ep"),
            P("ep", None, "tp"),
            P("ep", None, "tp"),
            P("ep", "tp", None),
            P(),
            P(None, "tp"),
            P(None, "tp"),
            P(None, "tp"),
            P(None, "tp"),
            P("tp", None),
            P(),
            P("ep", None),
            P("ep", None),
            P(None, ("ep", "tp")),
            P(None, ("ep", "tp")),
            P(("ep", "tp"), None),
        ),
        out_specs=P("ep", None),
        check_vma=False,
    )
```

```python
import functools

import jax
import jax.numpy as jnp
from jax import lax
from jax.experimental import pallas as pl
from jax.experimental.pallas import tpu as pltpu
from jax.sharding import PartitionSpec as P

HD = 64
EXPERTS = 8
CAP = 12
QUARTERS = 4
GROUP = 4
STEP_SEQS = 8
MESH = pl.DeviceIdType.MESH
F32 = jnp.float32
BF16 = jnp.bfloat16

eps = 1e-06


def normed(values, gain):
    floats = values.astype(F32)
    return floats * lax.rsqrt(jnp.mean(floats * floats, axis=-1, keepdims=True) + eps) * gain


def project(tok_ref, gain_ref, wq_ref, wk_ref, wv_ref, wf_ref, q_sc, lg_sc, kn_sc, vn_sc, heads):
    seqs = tok_ref.shape[0]
    lanes = wk_ref.shape[1]
    group = heads // (lanes // HD)
    per_slice = lanes // HD
    lane = lax.broadcasted_iota(jnp.int32, (seqs, lanes), 1)
    x = normed(tok_ref[...], gain_ref[...]).astype(BF16)
    gates = lax.dot_general(x, wf_ref[...], (((1,), (1,)), ((), ())), preferred_element_type=F32)
    gates = jnp.minimum(gates, 0.0) - jnp.log1p(jnp.exp(-jnp.abs(gates)))
    q = jnp.dot(x, wq_ref[...], preferred_element_type=F32).astype(BF16).astype(F32)
    kn_sc[...] = jnp.dot(x, wk_ref[...], preferred_element_type=F32).astype(BF16).astype(F32)
    vn_sc[...] = jnp.dot(x, wv_ref[...], preferred_element_type=F32).astype(BF16).astype(F32)
    for h in range(heads):
        base = (h // per_slice) * lanes
        part = q[:, base:base + lanes]
        at, want = h % per_slice, h // group
        if at != want:
            part = pltpu.roll(part, (want - at) * HD % lanes, 1)
        part = jnp.where(lane // HD == want, part, 0.0)
        q_sc[:, h, :] = part
        lg_sc[:, h, :] = jnp.broadcast_to(gates[:, h:h + 1], (seqs, lanes))


def attend(base, len_ref, k_ref, v_ref, g_ref, q_sc, lg_sc, kn_sc, vn_sc, mix_sc):
    heads, positions = g_ref.shape[1:]
    pos = lax.broadcasted_iota(jnp.int32, (heads, positions), 1)
    factor = HD ** (-0.5)
    group = [base + j for j in range(STEP_SEQS)]
    lengths = [len_ref[s] for s in group]
    queries = [q_sc[s] for s in group]
    scores = [
        lax.dot_general(
            q.astype(BF16), k_ref[s], (((1,), (1,)), ((), ())), preferred_element_type=F32
        )
        for s, q in zip(group, queries)
    ]
    latest = [
        jnp.sum(jnp.where(pos == n - 1, g_ref[s], 0.0), axis=-1, keepdims=True)
        for s, n in zip(group, lengths)
    ]
    own = [
        jnp.sum(q * kn_sc[pl.ds(s, 1), :], axis=-1, keepdims=True) * factor
        for s, q in zip(group, queries)
    ]
    scores = [
        jnp.where(pos < n, c * factor + (l + lg_sc[s][:, 0:1]) - g_ref[s], -jnp.inf)
        for s, n, c, l in zip(group, lengths, scores, latest)
    ]
    top = [jnp.maximum(jnp.max(c, axis=-1, keepdims=True), o) for c, o in zip(scores, own)]
    raised = [jnp.exp(c - m) for c, m in zip(scores, top)]
    own_raised = [jnp.exp(o - m) for o, m in zip(own, top)]
    inverse = [
        1.0 / (jnp.sum(r, axis=-1, keepdims=True) + o) for r, o in zip(raised, own_raised)
    ]
    weights = [(r * i).astype(BF16) for r, i in zip(raised, inverse)]
    mixed = [
        jnp.dot(w, v_ref[s], preferred_element_type=F32) for s, w in zip(group, weights)
    ]
    for s, m, o, i in zip(group, mixed, own_raised, inverse):
        mix_sc[s] = m + (o * i).astype(BF16).astype(F32) * vn_sc[pl.ds(s, 1), :]


def joined_heads(mix_sc):
    seqs, heads, lanes = mix_sc.shape
    per_slice = lanes // HD
    group = heads // per_slice
    lane = lax.broadcasted_iota(jnp.int32, (seqs, lanes), 1)
    pieces = []
    for base in range(0, heads, per_slice):
        joined = None
        for h in range(base, base + per_slice):
            part = mix_sc[:, h, :]
            at, want = h // group, h % per_slice
            if at != want:
                part = pltpu.roll(part, (want - at) * HD % lanes, 1)
            joined = part if joined is None else jnp.where(lane // HD == want, part, joined)
        pieces.append(joined.astype(BF16))
    return jnp.concatenate(pieces, axis=1)


def moe_kernel(
    n_ep, len_ref, mix_gain_ref, gain_ref, routes_ref, rw_ref, tok_hbm, wq_hbm, wk_hbm, wv_hbm,
    wf_hbm, k_hbm, v_hbm, g_hbm, wo_hbm, wg_hbm, wu_hbm, wd_hbm, out_ref,
    tok_ref, wq, wk, wv, wf, keys, values, gates, wo, wg, wu, wd,
    q_sc, lg_sc, kn_sc, vn_sc, mix_sc, part_ref, peer_part, residual, normal, outgoing, rows, x_sc, h_sc, stage, s_other, s_own,
    t_in, blocks, u_in, finals, returned,
    in_sem, kv_sem, w_sem, part_sem, col_send, fan_send, mate_send, row_recv, t_send, t_recv, u_send, u_recv,
    ret_send, ret_recv, out_sem,
):
    me = lax.axis_index("ep")
    t = lax.axis_index("tp")
    pieces = n_ep // EXPERTS
    e, p = me // pieces, lax.rem(me, pieces)
    mate = (me, 1 - t)
    order = (4, 3, 5, 2, 6, 1, 7)
    seqs, width = tok_ref.shape
    half = width // 2
    quarter = half // QUARTERS
    ff = wg_hbm.shape[1]

    def column(k):
        return lax.rem(e + k, EXPERTS)

    def peer(i):
        return lax.rem(p + i, pieces)

    head_copies = [
        pltpu.make_async_copy(src, dst, in_sem.at[i])
        for i, (src, dst) in enumerate((
            (tok_hbm, tok_ref), (wf_hbm, wf), (wq_hbm, wq), (wk_hbm, wk), (wv_hbm, wv),
            (wo_hbm, wo),
        ))
    ]
    for copy in head_copies[:-1]:
        copy.start()
    steps = seqs // STEP_SEQS

    def cache_copies(i):
        at = pl.ds(pl.multiple_of(i * STEP_SEQS, STEP_SEQS), STEP_SEQS)
        return [
            pltpu.make_async_copy(src.at[at], dst.at[at], kv_sem.at[n, i])
            for n, (src, dst) in enumerate(((k_hbm, keys), (g_hbm, gates), (v_hbm, values)))
        ]

    for i in range(steps):
        for copy in cache_copies(i):
            copy.start()
    head_copies[-1].start()
    weight_copies = [
        pltpu.make_async_copy(src, dst, w_sem.at[i])
        for i, (src, dst) in enumerate(((wg_hbm, wg), (wu_hbm, wu), (wd_hbm, wd)))
    ]
    for copy in weight_copies:
        copy.start()

    barrier = pltpu.get_barrier_semaphore()
    pl.semaphore_signal(barrier, inc=1, device_id=mate, device_id_type=MESH)
    for i in range(1, pieces):
        pl.semaphore_signal(barrier, inc=1, device_id=(e * pieces + peer(i), t), device_id_type=MESH)
    for k in range(1, EXPERTS):
        pl.semaphore_signal(barrier, inc=1, device_id=(column(k) * pieces + p, t), device_id_type=MESH)

    for copy in head_copies[:-1]:
        copy.wait()
    project(tok_ref, mix_gain_ref, wq, wk, wv, wf, q_sc, lg_sc, kn_sc, vn_sc, gates.shape[1])

    @pl.loop(0, steps)
    def _(i):
        for copy in cache_copies(i):
            copy.wait()
        attend(i * STEP_SEQS, len_ref, keys, values, gates, q_sc, lg_sc, kn_sc, vn_sc, mix_sc)

    head_copies[-1].wait()
    part_ref[...] = jnp.dot(
        joined_heads(mix_sc), wo[...], preferred_element_type=F32
    ).astype(BF16)

    pl.semaphore_wait(barrier, 1 + (pieces - 1) + (EXPERTS - 1))

    def send(src, dst, send_sem, recv_sem, device):
        copy = pltpu.make_async_remote_copy(
            src_ref=src, dst_ref=dst, send_sem=send_sem, recv_sem=recv_sem,
            device_id=device, device_id_type=MESH,
        )
        copy.start()
        return copy

    def arrived(dst, send_sem, recv_sem):
        pltpu.make_async_remote_copy(
            src_ref=dst, dst_ref=dst, send_sem=send_sem, recv_sem=recv_sem,
            device_id=mate, device_id_type=MESH,
        ).wait_recv()

    sent = [send(part_ref, peer_part, part_sem.at[0], part_sem.at[1], mate)]

    block = QUARTERS * CAP
    columns = EXPERTS * block
    spread = (columns, QUARTERS * seqs)
    row = lax.broadcasted_iota(jnp.int32, spread, 0)
    row_expert = row // block
    row_slot = lax.rem(row, CAP)
    same_quarter = lax.rem(row, block) // CAP == lax.broadcasted_iota(jnp.int32, spread, 1) // seqs
    tiled = lambda a: jnp.concatenate([a] * QUARTERS, axis=1)
    routes = tiled(routes_ref[...])
    shares = tiled(rw_ref[...])
    first, second = routes[0:1] == row_expert, routes[1:2] == row_expert
    named = jnp.where(first | second, 1.0, 0.0)
    square = (QUARTERS * seqs, QUARTERS * seqs)
    earlier = lax.broadcasted_iota(jnp.int32, square, 0)
    before = jnp.where(
        earlier < lax.rem(lax.broadcasted_iota(jnp.int32, square, 1), seqs), 1.0, 0.0
    )
    slot = jnp.dot(named.astype(BF16), before.astype(BF16), preferred_element_type=F32)
    chosen = jnp.where(same_quarter & (slot == row_slot.astype(F32)), named, 0.0)
    weight = jnp.where(first, shares[0:1], jnp.where(second, shares[1:2], 0.0)) * chosen
    dispatch = chosen.astype(BF16)
    weight_high = weight.astype(BF16)
    weight_low = (weight - weight_high.astype(F32)).astype(BF16)

    size = GROUP * block
    out_row = lax.broadcasted_iota(jnp.int32, (size, size), 0)
    in_row = lax.broadcasted_iota(jnp.int32, (size, size), 1)

    def unpacked(r):
        q = r // (GROUP * CAP)
        i = lax.rem(r, GROUP * CAP) // CAP
        return i * block + q * CAP + lax.rem(r, CAP)

    unpack = jnp.where(in_row == unpacked(out_row), 1.0, 0.0).astype(BF16)
    pack = jnp.where(out_row == unpacked(in_row), 1.0, 0.0).astype(BF16)

    arrived(peer_part, part_sem.at[0], part_sem.at[1])
    total = tok_ref[...].astype(F32) + (part_ref[...].astype(F32) + peer_part[...].astype(F32))
    rounded = total.astype(BF16)
    residual[...] = rounded
    normal[...] = normed(rounded, gain_ref[...]).astype(BF16)

    start = pl.multiple_of(t * half, half)
    mine = normal[:, pl.ds(start, half)]
    stacked = jnp.concatenate(
        [mine[:, q * quarter:(q + 1) * quarter] for q in range(QUARTERS)], axis=0
    )
    outgoing[...] = lax.dot_general(
        dispatch, stacked, (((1,), (0,)), ((), ())), preferred_element_type=F32
    ).astype(BF16).reshape(EXPERTS, block, quarter)

    own_row = p * EXPERTS + e
    for n, k in enumerate(order):
        a = column(k)
        sent.append(send(outgoing.at[a], rows.at[own_row, t], col_send.at[n],
                         row_recv.at[own_row, t], (a * pieces + p, t)))
    fans = 0
    mates = 0

    def fan(src, r):
        nonlocal fans
        for i in range(1, pieces):
            sent.append(send(src, rows.at[r, t], fan_send.at[fans], row_recv.at[r, t],
                             (e * pieces + peer(i), t)))
            fans += 1

    def to_mate(src, r):
        nonlocal mates
        sent.append(send(src, rows.at[r, t], mate_send.at[mates], row_recv.at[r, t], mate))
        mates += 1

    fan(outgoing.at[e], own_row)
    to_mate(outgoing.at[e], own_row)
    rows[own_row, t] = outgoing[e]
    inbound = [lax.rem(e + EXPERTS - k, EXPERTS) for k in order]
    for n, a in enumerate(inbound):
        r = p * EXPERTS + a
        arrived(rows.at[r, t], col_send.at[0], row_recv.at[r, t])
        fan(rows.at[r, t], r)
        to_mate(rows.at[r, t], r)
    for a in [e] + inbound:
        for i in range(1, pieces):
            r = peer(i) * EXPERTS + a
            arrived(rows.at[r, t], col_send.at[0], row_recv.at[r, t])
            to_mate(rows.at[r, t], r)
    for i in range(pieces):
        for a in [e] + inbound:
            r = peer(i) * EXPERTS + a
            arrived(rows.at[r, 1 - t], col_send.at[0], row_recv.at[r, 1 - t])

    groups = n_ep // GROUP
    group_rows = GROUP * CAP
    for g in range(groups):
        for h in range(2):
            packed = rows[g * GROUP:(g + 1) * GROUP, h].reshape(size, quarter)
            moved = jnp.dot(unpack, packed, preferred_element_type=F32).astype(BF16)
            for q in range(QUARTERS):
                x_sc[g * group_rows:(g + 1) * group_rows,
                     h * half + q * quarter:h * half + (q + 1) * quarter] = (
                    moved[q * group_rows:(q + 1) * group_rows])

    weight_copies[0].wait()
    weight_copies[1].wait()
    chunk = 256

    @pl.loop(0, ff // chunk)
    def _(c):
        at = pl.ds(pl.multiple_of(c * chunk, chunk), chunk)
        x = x_sc[...]
        gate = jnp.dot(x, wg[:, at], preferred_element_type=F32)
        up = jnp.dot(x, wu[:, at], preferred_element_type=F32)
        h_sc[:, at] = (gate * (1.0 / (1.0 + jnp.exp(-gate))) * up).astype(BF16)

    weight_copies[2].wait()

    def down(h, into):
        for q in range(QUARTERS):
            at = pl.ds(pl.multiple_of(h * half + q * quarter, quarter), quarter)
            y = jnp.dot(h_sc[...], wd[:, at], preferred_element_type=F32).astype(BF16)
            for g in range(groups):
                stage[g, q * group_rows:(q + 1) * group_rows] = (
                    y[g * group_rows:(g + 1) * group_rows])
        for g in range(groups):
            into[g * GROUP:(g + 1) * GROUP] = jnp.dot(
                pack, stage[g], preferred_element_type=F32
            ).astype(BF16).reshape(GROUP, block, quarter)

    down(1 - t, s_other)
    turns = list(range(1, pieces)) + [0]
    for i in turns:
        at = pl.ds(peer(i) * EXPERTS, EXPERTS)
        sent.append(send(s_other.at[at], t_in.at[at], t_send.at[i], t_recv.at[i], mate))
    down(t, s_own)
    backward = [column(k) for k in order] + [e]
    for i in turns:
        at = pl.ds(peer(i) * EXPERTS, EXPERTS)
        arrived(t_in.at[at], t_send.at[0], t_recv.at[i])
        for n, a in enumerate(backward):
            r = peer(i) * EXPERTS + a
            blocks[r] = (s_own[r].astype(F32) + t_in[r].astype(F32)).astype(BF16)
            if i > 0:
                sent.append(send(blocks.at[r], u_in.at[i - 1, a], u_send.at[i - 1, n],
                                 u_recv.at[i - 1, a], (e * pieces + peer(i), t)))
    for n, a in enumerate(backward):
        summed = blocks[p * EXPERTS + a].astype(F32)
        for i in range(1, pieces):
            arrived(u_in.at[i - 1, a], u_send.at[0, 0], u_recv.at[i - 1, a])
            summed = summed + u_in[i - 1, a].astype(F32)
        finals[a] = summed.astype(BF16)
        if n < len(order):
            sent.append(send(finals.at[a], returned.at[e], ret_send.at[n], ret_recv.at[e],
                             (a * pieces + p, t)))
    returned[e] = finals[e]
    for a in inbound:
        arrived(returned.at[a], ret_send.at[0], ret_recv.at[a])
    back = returned[...].reshape(columns, quarter)
    over_rows = (((0,), (0,)), ((), ()))
    mixture = (
        lax.dot_general(weight_high, back, over_rows, preferred_element_type=F32)
        + lax.dot_general(weight_low, back, over_rows, preferred_element_type=F32)
    )
    for q in range(QUARTERS):
        at = pl.ds(pl.multiple_of(start + q * quarter, quarter), quarter)
        out_ref[:, at] = (
            residual[:, at].astype(F32) + mixture[q * seqs:(q + 1) * seqs]
        ).astype(BF16)
    here = pl.ds(start, half)
    there = pl.ds(pl.multiple_of((1 - t) * half, half), half)
    sent.append(send(out_ref.at[:, here], out_ref.at[:, here], out_sem.at[0], out_sem.at[1], mate))
    arrived(out_ref.at[:, there], out_sem.at[0], out_sem.at[1])
    for copy in sent:
        copy.wait_send()


def on_device(
    n_ep, tokens, lengths, key_cache, value_cache, gate_cache, mix_gain, query_weight, key_weight,
    value_weight, forget_weight, out_weight, expert_gain, routes, route_weights, expert_gate,
    expert_up, expert_down,
):
    seqs, width = tokens.shape
    heads = gate_cache.shape[1]
    lanes = key_cache.shape[2]
    pieces = n_ep // EXPERTS
    half = width // 2
    quarter = half // QUARTERS
    block = QUARTERS * CAP
    ff = expert_gate.shape[1]
    count = n_ep * CAP
    vmem = pl.BlockSpec(memory_space=pltpu.VMEM)
    smem = pl.BlockSpec(memory_space=pltpu.SMEM)
    hbm = pl.BlockSpec(memory_space=pl.ANY)
    dma = lambda *s: pltpu.SemaphoreType.DMA(s)
    buf = lambda *s: pltpu.VMEM(s, BF16)
    copied = (
        tokens, query_weight, key_weight, value_weight, forget_weight.T, key_cache, value_cache,
        gate_cache, out_weight, expert_gate, expert_up, expert_down,
    )
    return pl.pallas_call(
        functools.partial(moe_kernel, n_ep),
        out_shape=jax.ShapeDtypeStruct((seqs, width), BF16),
        in_specs=[smem] + [vmem] * 4 + [hbm] * len(copied),
        out_specs=vmem,
        scratch_shapes=[pltpu.VMEM(a.shape, a.dtype) for a in copied] + [
            pltpu.VMEM((seqs, heads, lanes), F32),
            pltpu.VMEM((seqs, heads, lanes), F32),
            pltpu.VMEM((seqs, lanes), F32),
            pltpu.VMEM((seqs, lanes), F32),
            pltpu.VMEM((seqs, heads, lanes), F32),
            buf(seqs, width), buf(seqs, width), buf(seqs, width), buf(seqs, width),
            buf(EXPERTS, block, quarter),
            buf(n_ep, 2, block, quarter),
            buf(count, width), buf(count, ff),
            buf(n_ep // GROUP, GROUP * block, quarter),
            buf(n_ep, block, quarter), buf(n_ep, block, quarter),
            buf(n_ep, block, quarter), buf(n_ep, block, quarter),
            buf(max(1, pieces - 1), EXPERTS, block, quarter),
            buf(EXPERTS, block, quarter), buf(EXPERTS, block, quarter),
            dma(6), dma(3, seqs // STEP_SEQS),
            dma(3), dma(2), dma(EXPERTS), dma(max(1, EXPERTS * (pieces - 1))), dma(n_ep),
            dma(n_ep, 2), dma(pieces), dma(pieces),
            dma(max(1, pieces - 1), EXPERTS), dma(max(1, pieces - 1), EXPERTS),
            dma(EXPERTS), dma(EXPERTS), dma(2),
        ],
        compiler_params=pltpu.CompilerParams(
            collective_id=0, has_side_effects=True, vmem_limit_bytes=67043328
        ),
        name="layer",
    )(lengths, mix_gain.reshape(1, width), expert_gain.reshape(1, width), routes.T,
      route_weights.T, *copied)


def solution(mesh):
    return jax.shard_map(
        functools.partial(on_device, mesh.shape["ep"]),
        mesh=mesh,
        in_specs=(
            P("ep", None),
            P("ep"),
            P("ep", None, "tp"),
            P("ep", None, "tp"),
            P("ep", "tp", None),
            P(),
            P(None, "tp"),
            P(None, "tp"),
            P(None, "tp"),
            P(None, "tp"),
            P("tp", None),
            P(),
            P("ep", None),
            P("ep", None),
            P(None, ("ep", "tp")),
            P(None, ("ep", "tp")),
            P(("ep", "tp"), None),
        ),
        out_specs=P("ep", None),
        check_vma=False,
    )
```

```python
import functools

import jax
import jax.numpy as jnp
from jax import lax
from jax.experimental import pallas as pl
from jax.experimental.pallas import tpu as pltpu
from jax.sharding import PartitionSpec as P

HD = 64
EXPERTS = 8
CAP = 12
QUARTERS = 4
GROUP = 4
STEP_SEQS = 16
MESH = pl.DeviceIdType.MESH
F32 = jnp.float32
BF16 = jnp.bfloat16

eps = 1e-06


def normed(values, gain):
    floats = values.astype(F32)
    return floats * lax.rsqrt(jnp.mean(floats * floats, axis=-1, keepdims=True) + eps) * gain


def project(tok_ref, gain_ref, wq_ref, wk_ref, wv_ref, wf_ref, q_sc, lg_sc, kn_sc, vn_sc, heads):
    seqs = tok_ref.shape[0]
    lanes = wk_ref.shape[1]
    group = heads // (lanes // HD)
    per_slice = lanes // HD
    lane = lax.broadcasted_iota(jnp.int32, (seqs, lanes), 1)
    x = normed(tok_ref[...], gain_ref[...]).astype(BF16)
    gates = lax.dot_general(x, wf_ref[...], (((1,), (1,)), ((), ())), preferred_element_type=F32)
    gates = jnp.minimum(gates, 0.0) - jnp.log1p(jnp.exp(-jnp.abs(gates)))
    q = jnp.dot(x, wq_ref[...], preferred_element_type=F32).astype(BF16).astype(F32)
    kn_sc[...] = jnp.dot(x, wk_ref[...], preferred_element_type=F32).astype(BF16).astype(F32)
    vn_sc[...] = jnp.dot(x, wv_ref[...], preferred_element_type=F32).astype(BF16).astype(F32)
    for h in range(heads):
        base = (h // per_slice) * lanes
        part = q[:, base:base + lanes]
        at, want = h % per_slice, h // group
        if at != want:
            part = pltpu.roll(part, (want - at) * HD % lanes, 1)
        part = jnp.where(lane // HD == want, part, 0.0)
        q_sc[:, h, :] = part
        lg_sc[:, h, :] = jnp.broadcast_to(gates[:, h:h + 1], (seqs, lanes))


def attend(base, len_ref, k_ref, v_ref, g_ref, q_sc, lg_sc, kn_sc, vn_sc, mix_sc):
    heads, positions = g_ref.shape[1:]
    pos = lax.broadcasted_iota(jnp.int32, (heads, positions), 1)
    factor = HD ** (-0.5)
    group = [base + j for j in range(STEP_SEQS)]
    lengths = [len_ref[s] for s in group]
    queries = [q_sc[s] for s in group]
    scores = [
        lax.dot_general(
            q.astype(BF16), k_ref[s], (((1,), (1,)), ((), ())), preferred_element_type=F32
        )
        for s, q in zip(group, queries)
    ]
    latest = [
        jnp.sum(jnp.where(pos == n - 1, g_ref[s], 0.0), axis=-1, keepdims=True)
        for s, n in zip(group, lengths)
    ]
    own = [
        jnp.sum(q * kn_sc[pl.ds(s, 1), :], axis=-1, keepdims=True) * factor
        for s, q in zip(group, queries)
    ]
    scores = [
        jnp.where(pos < n, c * factor + (l + lg_sc[s][:, 0:1]) - g_ref[s], -jnp.inf)
        for s, n, c, l in zip(group, lengths, scores, latest)
    ]
    top = [jnp.maximum(jnp.max(c, axis=-1, keepdims=True), o) for c, o in zip(scores, own)]
    raised = [jnp.exp(c - m) for c, m in zip(scores, top)]
    own_raised = [jnp.exp(o - m) for o, m in zip(own, top)]
    inverse = [
        1.0 / (jnp.sum(r, axis=-1, keepdims=True) + o) for r, o in zip(raised, own_raised)
    ]
    weights = [(r * i).astype(BF16) for r, i in zip(raised, inverse)]
    mixed = [
        jnp.dot(w, v_ref[s], preferred_element_type=F32) for s, w in zip(group, weights)
    ]
    for s, m, o, i in zip(group, mixed, own_raised, inverse):
        mix_sc[s] = m + (o * i).astype(BF16).astype(F32) * vn_sc[pl.ds(s, 1), :]


def joined_heads(mix_sc):
    seqs, heads, lanes = mix_sc.shape
    per_slice = lanes // HD
    group = heads // per_slice
    lane = lax.broadcasted_iota(jnp.int32, (seqs, lanes), 1)
    pieces = []
    for base in range(0, heads, per_slice):
        joined = None
        for h in range(base, base + per_slice):
            part = mix_sc[:, h, :]
            at, want = h // group, h % per_slice
            if at != want:
                part = pltpu.roll(part, (want - at) * HD % lanes, 1)
            joined = part if joined is None else jnp.where(lane // HD == want, part, joined)
        pieces.append(joined.astype(BF16))
    return jnp.concatenate(pieces, axis=1)


def moe_kernel(
    n_ep, len_ref, mix_gain_ref, gain_ref, routes_ref, rw_ref, tok_hbm, wq_hbm, wk_hbm, wv_hbm,
    wf_hbm, k_hbm, v_hbm, g_hbm, wo_hbm, wg_hbm, wu_hbm, wd_hbm, out_ref,
    tok_ref, wq, wk, wv, wf, keys, values, gates, wo, wg, wu, wd,
    q_sc, lg_sc, kn_sc, vn_sc, mix_sc, part_ref, peer_part, residual, normal, outgoing, rows, x_sc, h_sc, stage, s_other, s_own,
    t_in, blocks, u_in, finals, returned,
    in_sem, kv_sem, w_sem, part_sem, col_send, fan_send, mate_send, row_recv, t_send, t_recv, u_send, u_recv,
    ret_send, ret_recv, out_sem,
):
    me = lax.axis_index("ep")
    t = lax.axis_index("tp")
    pieces = n_ep // EXPERTS
    e, p = me // pieces, lax.rem(me, pieces)
    mate = (me, 1 - t)
    order = (4, 3, 5, 2, 6, 1, 7)
    seqs, width = tok_ref.shape
    half = width // 2
    quarter = half // QUARTERS
    ff = wg_hbm.shape[1]

    def column(k):
        return lax.rem(e + k, EXPERTS)

    def peer(i):
        return lax.rem(p + i, pieces)

    head_copies = [
        pltpu.make_async_copy(src, dst, in_sem.at[i])
        for i, (src, dst) in enumerate((
            (tok_hbm, tok_ref), (wf_hbm, wf), (wq_hbm, wq), (wk_hbm, wk), (wv_hbm, wv),
            (wo_hbm, wo),
        ))
    ]
    for copy in head_copies[:-1]:
        copy.start()
    steps = seqs // STEP_SEQS

    def cache_copies(i):
        at = pl.ds(pl.multiple_of(i * STEP_SEQS, STEP_SEQS), STEP_SEQS)
        return [
            pltpu.make_async_copy(src.at[at], dst.at[at], kv_sem.at[n, i])
            for n, (src, dst) in enumerate(((k_hbm, keys), (g_hbm, gates), (v_hbm, values)))
        ]

    for i in range(steps):
        for copy in cache_copies(i):
            copy.start()
    head_copies[-1].start()
    weight_copies = [
        pltpu.make_async_copy(src, dst, w_sem.at[i])
        for i, (src, dst) in enumerate(((wg_hbm, wg), (wu_hbm, wu), (wd_hbm, wd)))
    ]

    barrier = pltpu.get_barrier_semaphore()
    pl.semaphore_signal(barrier, inc=1, device_id=mate, device_id_type=MESH)
    for i in range(1, pieces):
        pl.semaphore_signal(barrier, inc=1, device_id=(e * pieces + peer(i), t), device_id_type=MESH)
    for k in range(1, EXPERTS):
        pl.semaphore_signal(barrier, inc=1, device_id=(column(k) * pieces + p, t), device_id_type=MESH)

    for copy in head_copies[:-1]:
        copy.wait()
    project(tok_ref, mix_gain_ref, wq, wk, wv, wf, q_sc, lg_sc, kn_sc, vn_sc, gates.shape[1])

    @pl.loop(0, steps)
    def _(i):
        for copy in cache_copies(i):
            copy.wait()
        attend(i * STEP_SEQS, len_ref, keys, values, gates, q_sc, lg_sc, kn_sc, vn_sc, mix_sc)

    for copy in weight_copies:
        copy.start()
    head_copies[-1].wait()
    part_ref[...] = jnp.dot(
        joined_heads(mix_sc), wo[...], preferred_element_type=F32
    ).astype(BF16)

    pl.semaphore_wait(barrier, 1 + (pieces - 1) + (EXPERTS - 1))

    def send(src, dst, send_sem, recv_sem, device):
        copy = pltpu.make_async_remote_copy(
            src_ref=src, dst_ref=dst, send_sem=send_sem, recv_sem=recv_sem,
            device_id=device, device_id_type=MESH,
        )
        copy.start()
        return copy

    def arrived(dst, send_sem, recv_sem):
        pltpu.make_async_remote_copy(
            src_ref=dst, dst_ref=dst, send_sem=send_sem, recv_sem=recv_sem,
            device_id=mate, device_id_type=MESH,
        ).wait_recv()

    sent = [send(part_ref, peer_part, part_sem.at[0], part_sem.at[1], mate)]

    block = QUARTERS * CAP
    columns = EXPERTS * block
    spread = (columns, QUARTERS * seqs)
    row = lax.broadcasted_iota(jnp.int32, spread, 0)
    row_expert = row // block
    row_slot = lax.rem(row, CAP)
    same_quarter = lax.rem(row, block) // CAP == lax.broadcasted_iota(jnp.int32, spread, 1) // seqs
    tiled = lambda a: jnp.concatenate([a] * QUARTERS, axis=1)
    routes = tiled(routes_ref[...])
    shares = tiled(rw_ref[...])
    first, second = routes[0:1] == row_expert, routes[1:2] == row_expert
    named = jnp.where(first | second, 1.0, 0.0)
    square = (QUARTERS * seqs, QUARTERS * seqs)
    earlier = lax.broadcasted_iota(jnp.int32, square, 0)
    before = jnp.where(
        earlier < lax.rem(lax.broadcasted_iota(jnp.int32, square, 1), seqs), 1.0, 0.0
    )
    slot = jnp.dot(named.astype(BF16), before.astype(BF16), preferred_element_type=F32)
    chosen = jnp.where(same_quarter & (slot == row_slot.astype(F32)), named, 0.0)
    weight = jnp.where(first, shares[0:1], jnp.where(second, shares[1:2], 0.0)) * chosen
    dispatch = chosen.astype(BF16)
    weight_high = weight.astype(BF16)
    weight_low = (weight - weight_high.astype(F32)).astype(BF16)

    size = GROUP * block
    out_row = lax.broadcasted_iota(jnp.int32, (size, size), 0)
    in_row = lax.broadcasted_iota(jnp.int32, (size, size), 1)

    def unpacked(r):
        q = r // (GROUP * CAP)
        i = lax.rem(r, GROUP * CAP) // CAP
        return i * block + q * CAP + lax.rem(r, CAP)

    unpack = jnp.where(in_row == unpacked(out_row), 1.0, 0.0).astype(BF16)
    pack = jnp.where(out_row == unpacked(in_row), 1.0, 0.0).astype(BF16)

    arrived(peer_part, part_sem.at[0], part_sem.at[1])
    total = tok_ref[...].astype(F32) + (part_ref[...].astype(F32) + peer_part[...].astype(F32))
    rounded = total.astype(BF16)
    residual[...] = rounded
    normal[...] = normed(rounded, gain_ref[...]).astype(BF16)

    start = pl.multiple_of(t * half, half)
    mine = normal[:, pl.ds(start, half)]
    stacked = jnp.concatenate(
        [mine[:, q * quarter:(q + 1) * quarter] for q in range(QUARTERS)], axis=0
    )
    outgoing[...] = lax.dot_general(
        dispatch, stacked, (((1,), (0,)), ((), ())), preferred_element_type=F32
    ).astype(BF16).reshape(EXPERTS, block, quarter)

    own_row = p * EXPERTS + e
    for n, k in enumerate(order):
        a = column(k)
        sent.append(send(outgoing.at[a], rows.at[own_row, t], col_send.at[n],
                         row_recv.at[own_row, t], (a * pieces + p, t)))
    fans = 0
    mates = 0

    def fan(src, r):
        nonlocal fans
        for i in range(1, pieces):
            sent.append(send(src, rows.at[r, t], fan_send.at[fans], row_recv.at[r, t],
                             (e * pieces + peer(i), t)))
            fans += 1

    def to_mate(src, r):
        nonlocal mates
        sent.append(send(src, rows.at[r, t], mate_send.at[mates], row_recv.at[r, t], mate))
        mates += 1

    fan(outgoing.at[e], own_row)
    to_mate(outgoing.at[e], own_row)
    rows[own_row, t] = outgoing[e]
    inbound = [lax.rem(e + EXPERTS - k, EXPERTS) for k in order]
    for n, a in enumerate(inbound):
        r = p * EXPERTS + a
        arrived(rows.at[r, t], col_send.at[0], row_recv.at[r, t])
        fan(rows.at[r, t], r)
        to_mate(rows.at[r, t], r)
    for a in [e] + inbound:
        for i in range(1, pieces):
            r = peer(i) * EXPERTS + a
            arrived(rows.at[r, t], col_send.at[0], row_recv.at[r, t])
            to_mate(rows.at[r, t], r)
    for i in range(pieces):
        for a in [e] + inbound:
            r = peer(i) * EXPERTS + a
            arrived(rows.at[r, 1 - t], col_send.at[0], row_recv.at[r, 1 - t])

    groups = n_ep // GROUP
    group_rows = GROUP * CAP
    for g in range(groups):
        for h in range(2):
            packed = rows[g * GROUP:(g + 1) * GROUP, h].reshape(size, quarter)
            moved = jnp.dot(unpack, packed, preferred_element_type=F32).astype(BF16)
            for q in range(QUARTERS):
                x_sc[g * group_rows:(g + 1) * group_rows,
                     h * half + q * quarter:h * half + (q + 1) * quarter] = (
                    moved[q * group_rows:(q + 1) * group_rows])

    weight_copies[0].wait()
    weight_copies[1].wait()
    chunk = 256

    @pl.loop(0, ff // chunk)
    def _(c):
        at = pl.ds(pl.multiple_of(c * chunk, chunk), chunk)
        x = x_sc[...]
        gate = jnp.dot(x, wg[:, at], preferred_element_type=F32)
        up = jnp.dot(x, wu[:, at], preferred_element_type=F32)
        h_sc[:, at] = (gate * (1.0 / (1.0 + jnp.exp(-gate))) * up).astype(BF16)

    weight_copies[2].wait()

    def down(h, into):
        for q in range(QUARTERS):
            at = pl.ds(pl.multiple_of(h * half + q * quarter, quarter), quarter)
            y = jnp.dot(h_sc[...], wd[:, at], preferred_element_type=F32).astype(BF16)
            for g in range(groups):
                stage[g, q * group_rows:(q + 1) * group_rows] = (
                    y[g * group_rows:(g + 1) * group_rows])
        for g in range(groups):
            into[g * GROUP:(g + 1) * GROUP] = jnp.dot(
                pack, stage[g], preferred_element_type=F32
            ).astype(BF16).reshape(GROUP, block, quarter)

    down(1 - t, s_other)
    turns = list(range(1, pieces)) + [0]
    for i in turns:
        at = pl.ds(peer(i) * EXPERTS, EXPERTS)
        sent.append(send(s_other.at[at], t_in.at[at], t_send.at[i], t_recv.at[i], mate))
    down(t, s_own)
    backward = [column(k) for k in order] + [e]
    for i in turns:
        at = pl.ds(peer(i) * EXPERTS, EXPERTS)
        arrived(t_in.at[at], t_send.at[0], t_recv.at[i])
        for n, a in enumerate(backward):
            r = peer(i) * EXPERTS + a
            blocks[r] = (s_own[r].astype(F32) + t_in[r].astype(F32)).astype(BF16)
            if i > 0:
                sent.append(send(blocks.at[r], u_in.at[i - 1, a], u_send.at[i - 1, n],
                                 u_recv.at[i - 1, a], (e * pieces + peer(i), t)))
    for n, a in enumerate(backward):
        summed = blocks[p * EXPERTS + a].astype(F32)
        for i in range(1, pieces):
            arrived(u_in.at[i - 1, a], u_send.at[0, 0], u_recv.at[i - 1, a])
            summed = summed + u_in[i - 1, a].astype(F32)
        finals[a] = summed.astype(BF16)
        if n < len(order):
            sent.append(send(finals.at[a], returned.at[e], ret_send.at[n], ret_recv.at[e],
                             (a * pieces + p, t)))
    returned[e] = finals[e]
    for a in inbound:
        arrived(returned.at[a], ret_send.at[0], ret_recv.at[a])
    back = returned[...].reshape(columns, quarter)
    over_rows = (((0,), (0,)), ((), ()))
    mixture = (
        lax.dot_general(weight_high, back, over_rows, preferred_element_type=F32)
        + lax.dot_general(weight_low, back, over_rows, preferred_element_type=F32)
    )
    for q in range(QUARTERS):
        at = pl.ds(pl.multiple_of(start + q * quarter, quarter), quarter)
        out_ref[:, at] = (
            residual[:, at].astype(F32) + mixture[q * seqs:(q + 1) * seqs]
        ).astype(BF16)
    here = pl.ds(start, half)
    there = pl.ds(pl.multiple_of((1 - t) * half, half), half)
    sent.append(send(out_ref.at[:, here], out_ref.at[:, here], out_sem.at[0], out_sem.at[1], mate))
    arrived(out_ref.at[:, there], out_sem.at[0], out_sem.at[1])
    for copy in sent:
        copy.wait_send()


def on_device(
    n_ep, tokens, lengths, key_cache, value_cache, gate_cache, mix_gain, query_weight, key_weight,
    value_weight, forget_weight, out_weight, expert_gain, routes, route_weights, expert_gate,
    expert_up, expert_down,
):
    seqs, width = tokens.shape
    heads = gate_cache.shape[1]
    lanes = key_cache.shape[2]
    pieces = n_ep // EXPERTS
    half = width // 2
    quarter = half // QUARTERS
    block = QUARTERS * CAP
    ff = expert_gate.shape[1]
    count = n_ep * CAP
    vmem = pl.BlockSpec(memory_space=pltpu.VMEM)
    smem = pl.BlockSpec(memory_space=pltpu.SMEM)
    hbm = pl.BlockSpec(memory_space=pl.ANY)
    dma = lambda *s: pltpu.SemaphoreType.DMA(s)
    buf = lambda *s: pltpu.VMEM(s, BF16)
    copied = (
        tokens, query_weight, key_weight, value_weight, forget_weight.T, key_cache, value_cache,
        gate_cache, out_weight, expert_gate, expert_up, expert_down,
    )
    return pl.pallas_call(
        functools.partial(moe_kernel, n_ep),
        out_shape=jax.ShapeDtypeStruct((seqs, width), BF16),
        in_specs=[smem] + [vmem] * 4 + [hbm] * len(copied),
        out_specs=vmem,
        scratch_shapes=[pltpu.VMEM(a.shape, a.dtype) for a in copied] + [
            pltpu.VMEM((seqs, heads, lanes), F32),
            pltpu.VMEM((seqs, heads, lanes), F32),
            pltpu.VMEM((seqs, lanes), F32),
            pltpu.VMEM((seqs, lanes), F32),
            pltpu.VMEM((seqs, heads, lanes), F32),
            buf(seqs, width), buf(seqs, width), buf(seqs, width), buf(seqs, width),
            buf(EXPERTS, block, quarter),
            buf(n_ep, 2, block, quarter),
            buf(count, width), buf(count, ff),
            buf(n_ep // GROUP, GROUP * block, quarter),
            buf(n_ep, block, quarter), buf(n_ep, block, quarter),
            buf(n_ep, block, quarter), buf(n_ep, block, quarter),
            buf(max(1, pieces - 1), EXPERTS, block, quarter),
            buf(EXPERTS, block, quarter), buf(EXPERTS, block, quarter),
            dma(6), dma(3, seqs // STEP_SEQS),
            dma(3), dma(2), dma(EXPERTS), dma(max(1, EXPERTS * (pieces - 1))), dma(n_ep),
            dma(n_ep, 2), dma(pieces), dma(pieces),
            dma(max(1, pieces - 1), EXPERTS), dma(max(1, pieces - 1), EXPERTS),
            dma(EXPERTS), dma(EXPERTS), dma(2),
        ],
        compiler_params=pltpu.CompilerParams(
            collective_id=0, has_side_effects=True, vmem_limit_bytes=67043328
        ),
        name="layer",
    )(lengths, mix_gain.reshape(1, width), expert_gain.reshape(1, width), routes.T,
      route_weights.T, *copied)


def solution(mesh):
    return jax.shard_map(
        functools.partial(on_device, mesh.shape["ep"]),
        mesh=mesh,
        in_specs=(
            P("ep", None),
            P("ep"),
            P("ep", None, "tp"),
            P("ep", None, "tp"),
            P("ep", "tp", None),
            P(),
            P(None, "tp"),
            P(None, "tp"),
            P(None, "tp"),
            P(None, "tp"),
            P("tp", None),
            P(),
            P("ep", None),
            P("ep", None),
            P(None, ("ep", "tp")),
            P(None, ("ep", "tp")),
            P(("ep", "tp"), None),
        ),
        out_specs=P("ep", None),
        check_vma=False,
    )
```
